32 devices in a mesh: sp: 8 (over z, core), tp: 4 (over y, x).
Axes of the slice: x: 2, y: 2, z: 4, core: 2. Of those that a mesh axis runs over, the one named last changes fastest.
Arguments:
- cotangent: bfloat16 [1024, 2048], P('sp'), may hold values from -6 to 6
- stream: bfloat16 [1024, 2048], P('sp'), may hold values from -6 to 6
- routes: int32 [1024, 2], P('sp'), may hold values from 0 to 3, all different within a row; in each aligned block of 128 rows (0 to 127, 128 to 255, ...) at most 80 rows name the same one
- route_weights: float32 [1024, 2], P('sp'), may hold values from 0.2 to 1
- gate_proj: bfloat16 [8, 2048, 2048], P('sp', None, 'tp'), may hold values from -0.125 to 0.125
- up_proj: bfloat16 [8, 2048, 2048], P('sp', None, 'tp'), may hold values from -0.125 to 0.125
- down_proj: bfloat16 [8, 2048, 2048], P('sp', 'tp'), may hold values from -0.09375 to 0.09375
- out_weight: bfloat16 [2048, 8192], P('sp', 'tp'), may hold values from -0.0625 to 0.0625
- queries: bfloat16 [1024, 4096], P('sp', 'tp'), may hold values from -6 to 6
- keys: bfloat16 [1024, 4096], P('sp', 'tp'), may hold values from -6 to 6
- values: bfloat16 [1024, 8192], P('sp', 'tp'), may hold values from -6 to 6
- decay_rate: float32 [16], P('tp'), may hold values from 0 to 1
Outputs:
- grad_gate: bfloat16 [8, 2048, 2048], P('sp', None, 'tp')
- grad_up: bfloat16 [8, 2048, 2048], P('sp', None, 'tp')
- grad_down: bfloat16 [8, 2048, 2048], P('sp', 'tp')
- grad_out_weight: float32 [2048, 8192], P('sp', 'tp')
- grad_queries: bfloat16 [1024, 4096], P('sp', 'tp')
- grad_keys: bfloat16 [1024, 4096], P('sp', 'tp')
- grad_values: bfloat16 [1024, 8192], P('sp', 'tp')
The draws below stay inside these ranges and needn't reach their ends.
Inputs may be any that keep to these rules, and one draw needn't show every extreme that they name: `routes`: each row names two different experts. In each block of 128 consecutive tokens no expert is named more than 80 times, and in some block of every draw one expert is named exactly 80 times.
All inputs are finite; a program needn't handle non-finite values.
Results may differ from the reference program's by a relative error of at most 0.006.
Values may be sent and summed in bfloat16 or wider, within the bound.
A program may use at most 128 MiB of HBM per device.

```python
import math
import jax
import jax.numpy as jnp
import numpy as np
from jax import lax

D = 2048
FF = 4096
HEADS = 16
DK = 256
DV = 512
TOP = 2
TOK_DEV = 128
EXPERTS = 4
CAP = 80
ROWS_EXP = 640
UNITS = 512
TOKENS = 1024
N_SP = 8


def draw_decay_rate(key, part):
    folded = jax.random.fold_in(key, 17)
    key_slow, key_fast, key_pick = jax.random.split(folded, 3)
    slow_rate = jnp.exp(jax.random.uniform(key_slow, (HEADS,), jnp.float32, math.log(0.2), math.log(2.0))) / TOKENS
    fast_rate = jnp.exp(jax.random.uniform(key_fast, (HEADS,), jnp.float32, math.log(0.025), math.log(0.08)))
    chosen = jax.random.uniform(key_pick, (HEADS,), jnp.float32) < 0.5
    return jnp.where(chosen, fast_rate, slow_rate).astype(jnp.float32)


def raised(values, rng, source, target, parts, factor):
    def block_of(position):
        return (jnp.arange(values.shape[position]) // (values.shape[position] // parts)).reshape((-1,) + (1,) * (values.ndim - 1 - position))

    near = jax.random.permutation(rng, parts)[block_of(target)]
    far = (block_of(target) + parts // 2) % parts
    return jnp.where((block_of(source) == near) | (block_of(source) == far), factor * values, values)


def levels(key, extent, pieces, low, largest):
    loudness = 1.0
    for dim, blocks in pieces:
        draws = jax.random.uniform(jax.random.fold_in(jax.random.fold_in(key, 6), dim), (blocks,), jnp.float32, low / len(pieces), largest / len(pieces))
        loudness = loudness * jnp.repeat(jnp.exp(draws), extent[dim] // blocks).reshape((-1,) + (1,) * (len(extent) - 1 - dim))
    return loudness


def assign_block(key, own, number, rows, number_of, top, most, lean):
    order = jax.random.permutation(key, number_of)
    heavy_load, common = portions_of(number_of, rows * top, most, lean, True), portions_of(number_of, rows * top, most, lean, False)
    places = jnp.arange(number_of)

    def named(tallies, turn):
        used = int((tallies > 0).sum())
        fixed = max(1, used // 4)
        shifted = fixed + (places - fixed + turn * (used - fixed)) % max(1, number_of - fixed)
        return jnp.zeros((number_of,), jnp.int32).at[order[jnp.where(places < fixed, places, shifted)]].set(jnp.asarray(tallies, jnp.int32))

    tallies = jnp.where(number % 4 == 0, named(heavy_load, number // 4), named(common, number - number // 4 - 1))
    mixed = jax.random.permutation(jax.random.fold_in(own, 3), number_of)
    source_of, sink = mixed[0:number_of // 2 * 2:2], mixed[1:number_of // 2 * 2:2]
    room = jnp.minimum(tallies[source_of] - 1, most - tallies[sink]) // 2
    room = jnp.where((source_of == order[0]) | (sink == order[0]) | (tallies[sink] == 0), 0, jnp.maximum(room, 0))
    shifted = jax.random.randint(jax.random.fold_in(own, 4), (number_of // 2,), 0, 1 << 20) % (room + 1)
    tallies = tallies.at[source_of].add(-shifted).at[sink].add(shifted)
    labels = jnp.searchsorted(jnp.cumsum(tallies), jnp.arange(rows * top), side="right").astype(jnp.int32)
    table = labels.reshape(top, rows).T
    table = table[jax.random.permutation(jax.random.fold_in(own, 1), rows)]
    turn = jax.random.randint(jax.random.fold_in(own, 2), (rows, 1), 0, top)
    return jnp.take_along_axis(table, (jnp.arange(top)[None, :] + turn) % top, axis=1)


def portions_of(number_of, total, limit, skew, full):
    weights = [(1 << 20) // math.isqrt(rank ** skew) + 1 for rank in range(1, number_of + 1)]
    largest = limit if full else min(limit, max(-(-total // number_of), total * weights[0] // sum(weights)))
    least = 1 if total - largest >= number_of - 1 else 0
    counts, rest = [largest] + [least] * (number_of - 1), total - largest - least * (number_of - 1)
    while rest > 0:
        movable = [i for i in range(1, number_of) if counts[i] < largest] or [i for i in range(1, number_of) if counts[i] < limit]
        whole, left = sum([weights[i] for i in movable]), rest
        for i in movable:
            extra = min(limit - counts[i], max(1, left * weights[i] // whole), rest)
            counts[i] = counts[i] + extra
            rest = rest - extra
    return np.array(counts)


def gaussian(key, shape, width, limit, cuts=(), kind=jnp.bfloat16):
    drawn = jax.random.normal(key, shape, jnp.float32) * width
    if len(cuts) > 0:
        drawn = levels(key, shape, cuts, -0.22, 0.18) * drawn
    return jnp.clip(drawn, min=-limit, max=limit).astype(kind)


def bell_draw_with(own_key, extent, spread, bound, pieces, heavy, kind=jnp.bfloat16):
    values = spread * jax.random.normal(own_key, extent, jnp.float32)
    if pieces:
        values = values * levels(own_key, extent, pieces, -0.22, 0.18)
    return jnp.clip(raised(values, jax.random.fold_in(own_key, 3), *heavy), -bound, bound).astype(kind)


def setup_inputs(seed: int = 0) -> dict:
    seeds = jax.random.split(jax.random.key(seed), 13)
    cotangent = bell_draw_with(seeds[0], (TOKENS, D), 1.0, 6.0, ((0, 8),), (0, 1, 8, 2.0))
    stream = gaussian(seeds[1], (TOKENS, D), 1.0, 6.0, ((0, 8),))
    routes_keys = jax.random.split(jax.random.fold_in(seeds[2], 1), TOKENS // TOK_DEV)
    routes_turns = jax.random.permutation(jax.random.fold_in(seeds[2], 3), TOKENS // TOK_DEV)
    routes = jax.vmap(lambda own, number: assign_block(jax.random.fold_in(seeds[2], 2), own, number, TOK_DEV, EXPERTS, TOP, CAP, 1))(routes_keys, routes_turns).reshape((TOKENS, TOP))
    route_weights = jnp.clip(0.2 + 0.8 * jax.random.uniform(seeds[3], (TOKENS, TOP), jnp.float32) ** levels(seeds[3], (TOKENS, TOP), ((0, 8),), -0.2, 0.2), 0.2, 1.0)
    gate_proj = gaussian(seeds[4], (2 * EXPERTS, D, FF // 2), D ** -0.5, 0.125, ((0, 8), (2, 4)))
    up_proj = gaussian(seeds[5], (2 * EXPERTS, D, FF // 2), D ** -0.5, 0.125, ((0, 8), (2, 4)))
    down_proj = gaussian(seeds[6], (2 * EXPERTS, FF // 2, D), FF ** -0.5, 0.09375, ((0, 8), (1, 4)))
    out_weight = gaussian(seeds[7], (D, HEADS * DV), (HEADS * DV) ** -0.5, 0.0625, ((0, 8), (1, 4)))
    queries = gaussian(seeds[8], (TOKENS, HEADS * DK), 1.0, 6.0, ((0, 8), (1, 4)))
    keys = gaussian(seeds[9], (TOKENS, HEADS * DK), 1.0, 6.0, ((0, 8), (1, 4)))
    values = gaussian(seeds[10], (TOKENS, HEADS * DV), 1.0, 6.0, ((0, 8), (1, 4)))
    decay_rate = draw_decay_rate(jax.random.fold_in(seeds[12], 71), 0)
    return dict(cotangent=cotangent, stream=stream, routes=routes, route_weights=route_weights, gate_proj=gate_proj, up_proj=up_proj, down_proj=down_proj, out_weight=out_weight, queries=queries, keys=keys, values=values, decay_rate=decay_rate)


NORM_EPS = 1.0
precise_setting = lax.Precision.HIGHEST

def silu_grad(pre_act):
    sigmoid = jax.nn.sigmoid(pre_act)
    return sigmoid * (1.0 + pre_act * (1.0 - sigmoid))

def retain(query_wide_float, key_wide_float, value_wide_float, decay_rate):
    head_count, seq_length, key_dim = query_wide_float.shape
    value_dim = value_wide_float.shape[2]
    blocks = seq_length // TOK_DEV
    local_steps = jnp.arange(TOK_DEV, dtype=jnp.float32)
    distance = local_steps[:, None] - local_steps[None, :]
    decay_mask_matrix = jnp.where(distance >= 0, jnp.exp(-decay_rate[:, None, None] * jnp.maximum(distance, 0.0)), 0.0)
    enter_decay = jnp.exp(-decay_rate[:, None] * (local_steps + 1.0))[:, :, None]
    leave_decay = jnp.exp(-decay_rate[:, None] * (TOK_DEV - 1.0 - local_steps))[:, :, None]
    block_decay = jnp.exp(-decay_rate * TOK_DEV)[:, None, None]

    def split_blocks(array):
        return array.reshape(head_count, blocks, TOK_DEV, array.shape[2]).transpose(1, 0, 2, 3)

    def advance(carry_state, inputs):
        query_tile_rows, key_tile_rows, value_block = inputs
        attention_scores = jnp.einsum('niv,nov->nio', query_tile_rows, key_tile_rows, precision=precise_setting) * decay_mask_matrix
        result = jnp.einsum('hlm,hme->hle', attention_scores, value_block, precision=precise_setting)
        result = result + enter_decay * jnp.einsum('hld,hde->hle', query_tile_rows, carry_state, precision=precise_setting)
        added = jnp.einsum('hld,hle->hde', key_tile_rows * leave_decay, value_block, precision=precise_setting)
        return (block_decay * carry_state + added, result)
    state_zero = jnp.zeros((head_count, key_dim, value_dim), jnp.float32)
    _, outputs = lax.scan(advance, state_zero, (split_blocks(query_wide_float), split_blocks(key_wide_float), split_blocks(value_wide_float)))
    return outputs.transpose(1, 0, 2, 3).reshape(head_count, seq_length, value_dim)

def normalize(retained):
    centered = retained - lax.optimization_barrier(jnp.mean(retained, axis=-1, keepdims=True))
    return centered * lax.rsqrt(lax.optimization_barrier(jnp.mean(centered * centered, axis=-1, keepdims=True)) + NORM_EPS)

def one_expert(inputs):
    cot_rows, in_rows, gate_full, up_full, down_full = inputs
    row_count = cot_rows.shape[0]
    pre_gate = jnp.dot(in_rows, gate_full, preferred_element_type=jnp.float32)
    pre_up = jnp.dot(in_rows, up_full, preferred_element_type=jnp.float32)
    active = jax.nn.silu(pre_gate)
    hidden = (active * pre_up).astype(jnp.bfloat16)
    grad_hidden = jnp.dot(cot_rows, down_full.T, preferred_element_type=jnp.float32)
    grad_pre_gate = (grad_hidden * pre_up * silu_grad(pre_gate)).astype(jnp.bfloat16)
    grad_pre_up = (grad_hidden * active).astype(jnp.bfloat16)
    grad_gate = jnp.dot(in_rows.T, grad_pre_gate, preferred_element_type=jnp.float32).astype(jnp.bfloat16)
    grad_up = jnp.dot(in_rows.T, grad_pre_up, preferred_element_type=jnp.float32).astype(jnp.bfloat16)
    grad_down = jnp.dot(hidden.T, cot_rows, preferred_element_type=jnp.float32).astype(jnp.bfloat16)
    groups = FF // UNITS
    gate_part = jnp.einsum('rgu,dgu->grd', grad_pre_gate.astype(jnp.float32).reshape(row_count, groups, UNITS), gate_full.astype(jnp.float32).reshape(D, groups, UNITS), precision=precise_setting)
    up_part = jnp.einsum('rgu,dgu->grd', grad_pre_up.astype(jnp.float32).reshape(row_count, groups, UNITS), up_full.astype(jnp.float32).reshape(D, groups, UNITS), precision=precise_setting)
    group_part = lax.optimization_barrier((gate_part + up_part).astype(jnp.bfloat16))
    grad_in = lax.optimization_barrier(jnp.sum(group_part.astype(jnp.float32), axis=0))
    return (grad_gate, grad_up, grad_down, grad_in)

def reference(cotangent, stream, routes, route_weights, gate_proj, up_proj, down_proj, out_weight, queries, keys, values, decay_rate):
    experts = N_SP // 2
    half_units = FF // 2
    assigned = TOK_DEV * TOP
    by_block = routes.reshape(N_SP, assigned)
    onehot = (by_block[:, :, None] == jnp.arange(experts, dtype=jnp.int32)[None, None, :]).astype(jnp.int32)
    slot_rank = lax.optimization_barrier(jnp.sum((jnp.cumsum(onehot, axis=1) - 1) * onehot, axis=2))
    buffer_row = (jnp.arange(N_SP, dtype=jnp.int32)[:, None] * CAP + slot_rank).reshape(-1).astype(jnp.int32)
    expert_of = by_block.reshape(-1).astype(jnp.int32)
    token_of = (jnp.arange(TOKENS * TOP, dtype=jnp.int32) // TOP).astype(jnp.int32)
    scaled = (route_weights[:, :, None] * cotangent[:, None, :].astype(jnp.float32)).reshape(TOKENS * TOP, D).astype(jnp.bfloat16)
    cot_buffer = jnp.zeros((experts, ROWS_EXP, D), jnp.bfloat16).at[expert_of, buffer_row].set(scaled)
    row_buffer = jnp.zeros((experts, ROWS_EXP, D), jnp.bfloat16).at[expert_of, buffer_row].set(stream[token_of])
    gate_full = gate_proj.reshape(experts, 2, D, half_units).transpose(0, 2, 1, 3).reshape(experts, D, FF)
    up_full = up_proj.reshape(experts, 2, D, half_units).transpose(0, 2, 1, 3).reshape(experts, D, FF)
    down_full = down_proj.reshape(experts, FF, D)
    grad_gate, grad_up, grad_down, grad_in = lax.map(one_expert, (cot_buffer, row_buffer, gate_full, up_full, down_full))
    grad_gate = grad_gate.reshape(experts, D, 2, half_units).transpose(0, 2, 1, 3).reshape(2 * experts, D, half_units)
    grad_up = grad_up.reshape(experts, D, 2, half_units).transpose(0, 2, 1, 3).reshape(2 * experts, D, half_units)
    grad_down = grad_down.reshape(2 * experts, half_units, D)
    routed_grad = lax.optimization_barrier(jnp.sum(grad_in[expert_of, buffer_row].reshape(TOKENS, TOP, D), axis=1))
    mid_grad = (cotangent.astype(jnp.float32) + routed_grad).astype(jnp.bfloat16)
    query_wide_float = queries.astype(jnp.float32).reshape(TOKENS, HEADS, DK).transpose(1, 0, 2)
    key_wide_float = keys.astype(jnp.float32).reshape(TOKENS, HEADS, DK).transpose(1, 0, 2)
    value_wide_float = values.astype(jnp.float32).reshape(TOKENS, HEADS, DV).transpose(1, 0, 2)

    def mixer(query_in, key_in, value_in):
        return normalize(retain(query_in, key_in * DK ** (-0.5), value_in, decay_rate))
    normed, pullback = jax.vjp(mixer, query_wide_float, key_wide_float, value_wide_float)
    mixed = normed.transpose(1, 0, 2).reshape(TOKENS, HEADS * DV).astype(jnp.bfloat16)
    grad_out_weight = jnp.dot(mid_grad.T, mixed, preferred_element_type=jnp.float32)
    grad_mixed = jnp.dot(mid_grad, out_weight, preferred_element_type=jnp.float32)
    query_gradient, key_gradient, grad_v = pullback(grad_mixed.reshape(TOKENS, HEADS, DV).transpose(1, 0, 2))
    grad_queries = query_gradient.transpose(1, 0, 2).reshape(TOKENS, HEADS * DK).astype(jnp.bfloat16)
    grad_keys = key_gradient.transpose(1, 0, 2).reshape(TOKENS, HEADS * DK).astype(jnp.bfloat16)
    grad_values = grad_v.transpose(1, 0, 2).reshape(TOKENS, HEADS * DV).astype(jnp.bfloat16)
    return (grad_gate, grad_up, grad_down, grad_out_weight, grad_queries, grad_keys, grad_values)
```

```python
import jax
import jax.numpy as jnp
from jax import lax
from jax.sharding import PartitionSpec as P

NORM_EPS = 1.0
F32 = jnp.float32
BF16 = jnp.bfloat16


def xor_send(block, axis, k):
    if k == 0:
        return block
    count = lax.axis_size(axis)
    return lax.ppermute(block, axis, [(i, i ^ k) for i in range(count)])


def gather_cols(block, axis):
    count = lax.axis_size(axis)
    me = lax.axis_index(axis)
    cols = block.shape[1]
    out = jnp.zeros((block.shape[0], count * cols), block.dtype)
    for k in range(count):
        out = lax.dynamic_update_slice_in_dim(out, xor_send(block, axis, k), (me ^ k) * cols, 1)
    return out


def neighbour_states(part, step_decay, axis, reverse):
    count = lax.axis_size(axis)
    me = lax.axis_index(axis)
    heads, rows, cols = part.shape
    piece = rows // count
    held = jnp.zeros((count, heads, piece, cols), part.dtype)
    for k in range(count):
        other = me ^ k
        send = lax.dynamic_slice_in_dim(part, other * piece, piece, 1)
        held = lax.dynamic_update_index_in_dim(held, xor_send(send, axis, k), other, 0)
    state = jnp.zeros((heads, piece, cols), F32)
    entering = [None] * count
    for place in reversed(range(count)) if reverse else range(count):
        entering[place] = state.astype(part.dtype)
        state = step_decay * state + held[place].astype(F32)
    entering = jnp.stack(entering)
    out = jnp.zeros_like(part)
    for k in range(count):
        other = me ^ k
        send = lax.dynamic_index_in_dim(entering, other, 0, False)
        out = lax.dynamic_update_slice_in_dim(out, xor_send(send, axis, k), other * piece, 1)
    return out


def mm(equation, a, b):
    return jnp.einsum(equation, a, b, preferred_element_type=F32)


def local(
    cotangent,
    stream,
    routes,
    route_weights,
    gate_proj,
    up_proj,
    down_proj,
    out_weight,
    queries,
    keys,
    values,
    decay_rate,
):
    tok_rows, model_width = cotangent.shape
    top_count = routes.shape[1]
    seq_devices = lax.axis_size("sp")
    tp_devices = lax.axis_size("tp")
    sp_me = lax.axis_index("sp")
    tp_me = lax.axis_index("tp")
    experts = seq_devices // 2
    slot_count = 5 * tok_rows // seq_devices
    half_slots = slot_count // 2
    half_rows = seq_devices * half_slots
    col_width = model_width // tp_devices
    heads_here = decay_rate.shape[0]
    key_dim = queries.shape[1] // heads_here
    value_dim = values.shape[1] // heads_here
    scale = key_dim ** (-0.5)
    along_cols = (((1,), (1,)), ((), ()))
    along_rows = (((0,), (0,)), ((), ()))

    weight_full = lax.all_gather(out_weight, "sp", axis=0, tiled=True)

    own_cot = lax.dynamic_slice_in_dim(cotangent, tp_me * col_width, col_width, 1)
    own_stream = lax.dynamic_slice_in_dim(stream, tp_me * col_width, col_width, 1)
    onehot = (routes.reshape(-1)[:, None] == jnp.arange(experts, dtype=jnp.int32)[None, :]).astype(
        jnp.int32
    )
    slot_rank = jnp.sum((jnp.cumsum(onehot, axis=0) - 1) * onehot, axis=1)
    target = (routes.reshape(-1) * slot_count + slot_rank).reshape(tok_rows, top_count)
    place = jnp.arange(half_rows, dtype=jnp.int32)
    slot_index = ((sp_me ^ (place // half_slots)) * half_slots + place % half_slots)[:, None]
    chosen = [slot_index == target[:, choice][None, :] for choice in range(top_count)]
    place_tokens = sum(one.astype(F32) for one in chosen).astype(BF16)
    place_pairs = jnp.concatenate([one.astype(BF16) for one in chosen], axis=1)
    scaled = jnp.concatenate(
        [
            (route_weights[:, choice][:, None] * own_cot.astype(F32)).astype(BF16)
            for choice in range(top_count)
        ],
        axis=0,
    )
    cot_send = jnp.dot(place_pairs, scaled, preferred_element_type=F32).astype(BF16)
    row_send = jnp.dot(place_tokens, own_stream, preferred_element_type=F32).astype(BF16)
    packed = jnp.stack(
        [
            cot_send.reshape(seq_devices, half_slots, col_width),
            row_send.reshape(seq_devices, half_slots, col_width),
        ],
        axis=1,
    )
    own_rows = jnp.stack([xor_send(packed[k], "sp", k) for k in range(seq_devices)], axis=1)
    own_rows = own_rows.reshape(2, half_rows, col_width)
    cot_rows = jnp.zeros((2 * half_rows, model_width), BF16)
    in_rows = jnp.zeros((2 * half_rows, model_width), BF16)
    for k in range(tp_devices):
        mine = xor_send(own_rows, "tp", k)
        both = jnp.concatenate([mine, xor_send(mine, "sp", 1)], axis=1)
        offset = (tp_me ^ k) * col_width
        cot_rows = lax.dynamic_update_slice_in_dim(cot_rows, both[0], offset, 1)
        in_rows = lax.dynamic_update_slice_in_dim(in_rows, both[1], offset, 1)

    def by_head(array, width):
        return array.reshape(tok_rows, heads_here, width).transpose(1, 0, 2)

    def flat(array):
        return array.transpose(1, 0, 2).reshape(tok_rows, -1).astype(BF16)

    query = by_head(queries, key_dim)
    key = by_head(keys, key_dim)
    value = by_head(values, value_dim)
    steps = jnp.arange(tok_rows, dtype=F32)
    distance = steps[:, None] - steps[None, :]
    decay_mask = jnp.where(
        distance >= 0, jnp.exp(-decay_rate[:, None, None] * jnp.maximum(distance, 0.0)), 0.0
    )
    decay_mask = decay_mask * scale
    enter_decay = jnp.exp(-decay_rate[:, None] * (steps + 1.0))[:, :, None]
    leave_decay = jnp.exp(-decay_rate[:, None] * (tok_rows - 1.0 - steps))[:, :, None]
    start_decay = jnp.exp(-decay_rate[:, None] * steps)[:, :, None]
    trailing_decay = jnp.exp(-decay_rate[:, None] * (tok_rows - steps))[:, :, None]
    block_decay = jnp.exp(-decay_rate * tok_rows)[:, None, None]
    left_key = (key.astype(F32) * (leave_decay * scale)).astype(BF16)
    carried = neighbour_states(
        mm("hld,hle->hde", left_key, value).astype(BF16), block_decay, "sp", False
    )
    scores = (mm("hid,hjd->hij", query, key) * decay_mask).astype(BF16)
    retained = mm("hlm,hme->hle", scores, value)
    retained = retained + enter_decay * mm("hld,hde->hle", query, carried)
    centered = retained - jnp.mean(retained, axis=-1, keepdims=True)
    inv_scale = lax.rsqrt(jnp.mean(centered * centered, axis=-1, keepdims=True) + NORM_EPS)
    normed = centered * inv_scale
    mixed_full = lax.all_gather(flat(normed), "sp", axis=0, tiled=True)

    gate_here = gate_proj[0]
    up_here = up_proj[0]
    down_here = down_proj[0]
    pre_gate = jnp.dot(in_rows, gate_here, preferred_element_type=F32)
    pre_up = jnp.dot(in_rows, up_here, preferred_element_type=F32)
    grad_hidden = lax.dot_general(cot_rows, down_here, along_cols, preferred_element_type=F32)
    sigmoid = jax.nn.sigmoid(pre_gate)
    active = pre_gate * sigmoid
    hidden = (active * pre_up).astype(BF16)
    grad_pre_gate = (
        grad_hidden * pre_up * (sigmoid * (1.0 + pre_gate * (1.0 - sigmoid)))
    ).astype(BF16)
    grad_pre_up = (grad_hidden * active).astype(BF16)

    def grad_in(low):
        rows = slice(low, low + half_rows)
        return lax.dot_general(
            grad_pre_gate[rows], gate_here, along_cols, preferred_element_type=F32
        ) + lax.dot_general(grad_pre_up[rows], up_here, along_cols, preferred_element_type=F32)

    from_partner = xor_send(grad_in(half_rows).astype(BF16), "sp", 1)
    partial_in = (grad_in(0) + from_partner.astype(F32)).astype(BF16)
    summed = jnp.zeros((half_rows, col_width), F32)
    for k in range(tp_devices):
        send = lax.dynamic_slice_in_dim(partial_in, (tp_me ^ k) * col_width, col_width, 1)
        summed = summed + xor_send(send, "tp", k).astype(F32)
    summed = summed.astype(BF16).reshape(seq_devices, half_slots, col_width)
    per_slot = jnp.stack([xor_send(summed[k], "sp", k) for k in range(seq_devices)])
    per_slot = per_slot.reshape(half_rows, col_width)
    token_grad = lax.dot_general(place_tokens, per_slot, along_rows, preferred_element_type=F32)
    mid_cols = (own_cot.astype(F32) + token_grad).astype(BF16)
    mid_grad = gather_cols(mid_cols, "tp")

    grad_gate = lax.dot_general(
        in_rows, grad_pre_gate, along_rows, preferred_element_type=F32
    ).astype(BF16)
    grad_up = lax.dot_general(
        in_rows, grad_pre_up, along_rows, preferred_element_type=F32
    ).astype(BF16)
    grad_down = lax.dot_general(hidden, cot_rows, along_rows, preferred_element_type=F32).astype(
        BF16
    )

    row_width = model_width // seq_devices
    mid_rows = jnp.zeros((seq_devices, tok_rows, row_width), BF16)
    for k in range(seq_devices):
        other = sp_me ^ k
        send = lax.dynamic_slice_in_dim(mid_grad, other * row_width, row_width, 1)
        mid_rows = lax.dynamic_update_index_in_dim(mid_rows, xor_send(send, "sp", k), other, 0)
    mid_rows = mid_rows.reshape(seq_devices * tok_rows, row_width)
    grad_out_weight = lax.dot_general(mid_rows, mixed_full, along_rows, preferred_element_type=F32)

    head_grad = jnp.dot(mid_grad, weight_full, preferred_element_type=F32)
    head_grad = head_grad.reshape(tok_rows, heads_here, value_dim).transpose(1, 0, 2)
    grad_retained = (
        inv_scale
        * (
            head_grad
            - jnp.mean(head_grad, axis=-1, keepdims=True)
            - normed * jnp.mean(head_grad * normed, axis=-1, keepdims=True)
        )
    ).astype(BF16)
    started_query = (query.astype(F32) * start_decay).astype(BF16)
    future = neighbour_states(
        mm("hld,hle->hde", started_query, grad_retained).astype(BF16), block_decay, "sp", True
    )
    score_grad = (mm("hle,hme->hlm", grad_retained, value) * decay_mask).astype(BF16)
    query_gradient = mm("hlm,hmd->hld", score_grad, key)
    query_gradient = query_gradient + enter_decay * mm("hle,hde->hld", grad_retained, carried)
    key_gradient = mm("hlm,hld->hmd", score_grad, query)
    key_gradient = key_gradient + (trailing_decay * scale) * mm("hme,hde->hmd", value, future)
    grad_v = mm("hlm,hle->hme", scores, grad_retained)
    grad_v = grad_v + (trailing_decay * scale) * mm("hmd,hde->hme", key, future)
    return (
        grad_gate[None],
        grad_up[None],
        grad_down[None],
        grad_out_weight,
        flat(query_gradient),
        flat(key_gradient),
        flat(grad_v),
    )


def solution(mesh):
    tokens = P("sp", None)
    cut = P("sp", "tp")
    wide = P("sp", None, "tp")
    tall = P("sp", "tp", None)
    in_specs = (tokens, tokens, tokens, tokens, wide, wide, tall, cut, cut, cut, cut, P("tp"))
    out_specs = (wide, wide, tall, cut, cut, cut, cut)
    return jax.shard_map(local, mesh=mesh, in_specs=in_specs, out_specs=out_specs, check_vma=False)
```

```python
import jax
import jax.numpy as jnp
from jax import lax
from jax.sharding import PartitionSpec as P

NORM_EPS = 1.0
F32 = jnp.float32
BF16 = jnp.bfloat16


def xor_send(block, axis, k):
    if k == 0:
        return block
    count = lax.axis_size(axis)
    return lax.ppermute(block, axis, [(i, i ^ k) for i in range(count)])


def gather_cols(block, axis):
    count = lax.axis_size(axis)
    me = lax.axis_index(axis)
    cols = block.shape[1]
    out = jnp.zeros((block.shape[0], count * cols), block.dtype)
    for k in range(count):
        out = lax.dynamic_update_slice_in_dim(out, xor_send(block, axis, k), (me ^ k) * cols, 1)
    return out


def entering_pieces(part, step_decay, axis, reverse):
    count = lax.axis_size(axis)
    me = lax.axis_index(axis)
    heads, rows, cols = part.shape
    piece = rows // count
    held = jnp.zeros((count, heads, piece, cols), part.dtype)
    for k in range(count):
        other = me ^ k
        send = lax.dynamic_slice_in_dim(part, other * piece, piece, 1)
        held = lax.dynamic_update_index_in_dim(held, xor_send(send, axis, k), other, 0)
    state = jnp.zeros((heads, piece, cols), F32)
    entering = [None] * count
    for place in reversed(range(count)) if reverse else range(count):
        entering[place] = state.astype(part.dtype)
        state = step_decay * state + held[place].astype(F32)
    return jnp.stack(entering)


def own_state(entering, axis):
    count, heads, piece, cols = entering.shape
    me = lax.axis_index(axis)
    out = jnp.zeros_like(entering)
    for k in range(count):
        other = me ^ k
        send = lax.dynamic_index_in_dim(entering, other, 0, False)
        out = lax.dynamic_update_index_in_dim(out, xor_send(send, axis, k), other, 0)
    return out.transpose(1, 0, 2, 3).reshape(heads, count * piece, cols)


def mm(equation, a, b):
    return jnp.einsum(equation, a, b, preferred_element_type=F32)


def local(
    cotangent,
    stream,
    routes,
    route_weights,
    gate_proj,
    up_proj,
    down_proj,
    out_weight,
    queries,
    keys,
    values,
    decay_rate,
):
    tok_rows, model_width = cotangent.shape
    top_count = routes.shape[1]
    seq_devices = lax.axis_size("sp")
    tp_devices = lax.axis_size("tp")
    sp_me = lax.axis_index("sp")
    tp_me = lax.axis_index("tp")
    experts = seq_devices // 2
    slot_count = 5 * tok_rows // seq_devices
    half_slots = slot_count // 2
    half_rows = seq_devices * half_slots
    col_width = model_width // tp_devices
    heads_here = decay_rate.shape[0]
    key_dim = queries.shape[1] // heads_here
    value_dim = values.shape[1] // heads_here
    scale = key_dim ** (-0.5)
    along_cols = (((1,), (1,)), ((), ()))
    along_rows = (((0,), (0,)), ((), ()))

    weight_full = lax.all_gather(out_weight, "sp", axis=0, tiled=True)

    own_cot = lax.dynamic_slice_in_dim(cotangent, tp_me * col_width, col_width, 1)
    own_stream = lax.dynamic_slice_in_dim(stream, tp_me * col_width, col_width, 1)
    onehot = (routes.reshape(-1)[:, None] == jnp.arange(experts, dtype=jnp.int32)[None, :]).astype(
        jnp.int32
    )
    slot_rank = jnp.sum((jnp.cumsum(onehot, axis=0) - 1) * onehot, axis=1)
    target = (routes.reshape(-1) * slot_count + slot_rank).reshape(tok_rows, top_count)
    place = jnp.arange(half_rows, dtype=jnp.int32)
    slot_index = ((sp_me ^ (place // half_slots)) * half_slots + place % half_slots)[:, None]
    chosen = [slot_index == target[:, choice][None, :] for choice in range(top_count)]
    place_tokens = sum(one.astype(F32) for one in chosen).astype(BF16)
    place_pairs = jnp.concatenate([one.astype(BF16) for one in chosen], axis=1)
    scaled = jnp.concatenate(
        [
            (route_weights[:, choice][:, None] * own_cot.astype(F32)).astype(BF16)
            for choice in range(top_count)
        ],
        axis=0,
    )
    cot_send = jnp.dot(place_pairs, scaled, preferred_element_type=F32).astype(BF16)
    row_send = jnp.dot(place_tokens, own_stream, preferred_element_type=F32).astype(BF16)
    packed = jnp.stack(
        [
            cot_send.reshape(seq_devices, half_slots, col_width),
            row_send.reshape(seq_devices, half_slots, col_width),
        ],
        axis=1,
    )
    own_rows = jnp.stack([xor_send(packed[k], "sp", k) for k in range(seq_devices)], axis=1)
    own_rows = own_rows.reshape(2, half_rows, col_width)
    cot_rows = jnp.zeros((2 * half_rows, model_width), BF16)
    in_rows = jnp.zeros((2 * half_rows, model_width), BF16)
    for k in range(tp_devices):
        mine = xor_send(own_rows, "tp", k)
        both = jnp.concatenate([mine, xor_send(mine, "sp", 1)], axis=1)
        offset = (tp_me ^ k) * col_width
        cot_rows = lax.dynamic_update_slice_in_dim(cot_rows, both[0], offset, 1)
        in_rows = lax.dynamic_update_slice_in_dim(in_rows, both[1], offset, 1)

    def by_head(array, width):
        return array.reshape(tok_rows, heads_here, width).transpose(1, 0, 2)

    def flat(array):
        return array.transpose(1, 0, 2).reshape(tok_rows, -1).astype(BF16)

    query = by_head(queries, key_dim)
    key = by_head(keys, key_dim)
    value = by_head(values, value_dim)
    steps = jnp.arange(tok_rows, dtype=F32)
    distance = steps[:, None] - steps[None, :]
    decay_mask = jnp.where(
        distance >= 0, jnp.exp(-decay_rate[:, None, None] * jnp.maximum(distance, 0.0)), 0.0
    )
    decay_mask = decay_mask * scale
    enter_decay = jnp.exp(-decay_rate[:, None] * (steps + 1.0))[:, :, None]
    leave_decay = jnp.exp(-decay_rate[:, None] * (tok_rows - 1.0 - steps))[:, :, None]
    start_decay = jnp.exp(-decay_rate[:, None] * steps)[:, :, None]
    trailing_decay = jnp.exp(-decay_rate[:, None] * (tok_rows - steps))[:, :, None]
    block_decay = jnp.exp(-decay_rate * tok_rows)[:, None, None]
    left_key = (key.astype(F32) * (leave_decay * scale)).astype(BF16)
    left_state = mm("hld,hle->hde", left_key, value).astype(BF16)
    left_state, _ = lax.optimization_barrier((left_state, own_rows))
    pieces = entering_pieces(left_state, block_decay, "sp", False)

    gate_here = gate_proj[0]
    up_here = up_proj[0]
    down_here = down_proj[0]
    pre_gate = jnp.dot(in_rows, gate_here, preferred_element_type=F32)
    pre_up = jnp.dot(in_rows, up_here, preferred_element_type=F32)
    grad_hidden = lax.dot_general(cot_rows, down_here, along_cols, preferred_element_type=F32)
    sigmoid = jax.nn.sigmoid(pre_gate)
    active = pre_gate * sigmoid
    hidden = (active * pre_up).astype(BF16)
    grad_pre_gate = (
        grad_hidden * pre_up * (sigmoid * (1.0 + pre_gate * (1.0 - sigmoid)))
    ).astype(BF16)
    grad_pre_up = (grad_hidden * active).astype(BF16)

    def grad_in(low):
        rows = slice(low, low + half_rows)
        return lax.dot_general(
            grad_pre_gate[rows], gate_here, along_cols, preferred_element_type=F32
        ) + lax.dot_general(grad_pre_up[rows], up_here, along_cols, preferred_element_type=F32)

    from_partner = xor_send(grad_in(half_rows).astype(BF16), "sp", 1)
    partial_in = (grad_in(0) + from_partner.astype(F32)).astype(BF16)
    partial_in, pieces = lax.optimization_barrier((partial_in, pieces))
    summed = jnp.zeros((half_rows, col_width), F32)
    for k in range(tp_devices):
        send = lax.dynamic_slice_in_dim(partial_in, (tp_me ^ k) * col_width, col_width, 1)
        summed = summed + xor_send(send, "tp", k).astype(F32)
    summed = summed.astype(BF16).reshape(seq_devices, half_slots, col_width)
    per_slot = jnp.stack([xor_send(summed[k], "sp", k) for k in range(seq_devices)])
    per_slot = per_slot.reshape(half_rows, col_width)
    token_grad = lax.dot_general(place_tokens, per_slot, along_rows, preferred_element_type=F32)
    mid_cols = (own_cot.astype(F32) + token_grad).astype(BF16)
    mid_grad = gather_cols(mid_cols, "tp")

    carried = own_state(pieces, "sp")
    scores = (mm("hid,hjd->hij", query, key) * decay_mask).astype(BF16)
    retained = mm("hlm,hme->hle", scores, value)
    retained = retained + enter_decay * mm("hld,hde->hle", query, carried)
    centered = retained - jnp.mean(retained, axis=-1, keepdims=True)
    inv_scale = lax.rsqrt(jnp.mean(centered * centered, axis=-1, keepdims=True) + NORM_EPS)
    normed = centered * inv_scale
    mixed_full = lax.all_gather(flat(normed), "sp", axis=0, tiled=True)

    grad_gate = lax.dot_general(
        in_rows, grad_pre_gate, along_rows, preferred_element_type=F32
    ).astype(BF16)
    grad_up = lax.dot_general(
        in_rows, grad_pre_up, along_rows, preferred_element_type=F32
    ).astype(BF16)
    grad_down = lax.dot_general(hidden, cot_rows, along_rows, preferred_element_type=F32).astype(
        BF16
    )

    head_grad = jnp.dot(mid_grad, weight_full, preferred_element_type=F32)
    head_grad = head_grad.reshape(tok_rows, heads_here, value_dim).transpose(1, 0, 2)
    grad_retained = (
        inv_scale
        * (
            head_grad
            - jnp.mean(head_grad, axis=-1, keepdims=True)
            - normed * jnp.mean(head_grad * normed, axis=-1, keepdims=True)
        )
    ).astype(BF16)
    started_query = (query.astype(F32) * start_decay).astype(BF16)
    back_state = mm("hld,hle->hde", started_query, grad_retained).astype(BF16)
    mid_late, back_state = lax.optimization_barrier((mid_grad, back_state))
    row_width = model_width // seq_devices
    mid_rows = jnp.zeros((seq_devices, tok_rows, row_width), BF16)
    for k in range(seq_devices):
        other = sp_me ^ k
        send = lax.dynamic_slice_in_dim(mid_late, other * row_width, row_width, 1)
        mid_rows = lax.dynamic_update_index_in_dim(mid_rows, xor_send(send, "sp", k), other, 0)
    mid_rows = mid_rows.reshape(seq_devices * tok_rows, row_width)
    grad_out_weight = lax.dot_general(mid_rows, mixed_full, along_rows, preferred_element_type=F32)

    future = own_state(entering_pieces(back_state, block_decay, "sp", True), "sp")
    score_grad = (mm("hle,hme->hlm", grad_retained, value) * decay_mask).astype(BF16)
    query_gradient = mm("hlm,hmd->hld", score_grad, key)
    query_gradient = query_gradient + enter_decay * mm("hle,hde->hld", grad_retained, carried)
    key_gradient = mm("hlm,hld->hmd", score_grad, query)
    key_gradient = key_gradient + (trailing_decay * scale) * mm("hme,hde->hmd", value, future)
    grad_v = mm("hlm,hle->hme", scores, grad_retained)
    grad_v = grad_v + (trailing_decay * scale) * mm("hmd,hde->hme", key, future)
    return (
        grad_gate[None],
        grad_up[None],
        grad_down[None],
        grad_out_weight,
        flat(query_gradient),
        flat(key_gradient),
        flat(grad_v),
    )


def solution(mesh):
    tokens = P("sp", None)
    cut = P("sp", "tp")
    wide = P("sp", None, "tp")
    tall = P("sp", "tp", None)
    in_specs = (tokens, tokens, tokens, tokens, wide, wide, tall, cut, cut, cut, cut, P("tp"))
    out_specs = (wide, wide, tall, cut, cut, cut, cut)
    return jax.shard_map(local, mesh=mesh, in_specs=in_specs, out_specs=out_specs, check_vma=False)
```
